32 devices in a mesh: ep: 8 (over z, core), tp: 4 (over y, x).
Axes of the slice: x: 2, y: 2, z: 4, core: 2. Of those that a mesh axis runs over, the one named last changes fastest.
Arguments:
- resid: bfloat16 [32, 2048], P('ep', 'tp'), may hold values from -6 to 6
- cache_key: bfloat16 [32, 8, 224, 256], P(('ep', 'tp')), may hold values from -360 to 360
- cache_value: bfloat16 [32, 8, 224, 256], P(('ep', 'tp')), may hold values from -6 to 6
- lengths: int32 [32], P(('ep', 'tp')), may hold values from 28 to 224
- lambdas: float32 [8], replicated, may hold values from 0.3 to 0.8
- mix_gain: float32 [2048], replicated, may hold values from 0.1 to 1.9
- query_gain: float32 [128], replicated, may hold values from 0.1 to 1.9
- key_gain: float32 [128], replicated, may hold values from 0.1 to 1.9
- sub_gain: float32 [256], replicated, may hold values from 0.1 to 1.9
- ffn_gain: float32 [2048], replicated, may hold values from 0.1 to 1.9
- w_query: bfloat16 [2048, 2048], P(None, 'tp'), may hold values from -0.125 to 0.125
- w_key: bfloat16 [2048, 2048], P(None, 'tp'), may hold values from -0.125 to 0.125
- w_value: bfloat16 [2048, 2048], P(None, 'tp'), may hold values from -0.125 to 0.125
- w_out: bfloat16 [2048, 2048], P(None, 'tp'), may hold values from -0.125 to 0.125
- routes: int32 [32, 2], P('ep'), may hold values from 0 to 7, all different within a row; in each aligned block of 4 rows (0 to 3, 4 to 7, ...) at most 4 rows name the same one
- route_weights: float32 [32, 2], P('ep'), may hold values from 0.2 to 0.8
- w_gate: bfloat16 [8, 2048, 4096], P('ep', None, 'tp'), may hold values from -0.125 to 0.125
- w_up: bfloat16 [8, 2048, 4096], P('ep', None, 'tp'), may hold values from -0.125 to 0.125
- w_down: bfloat16 [8, 4096, 2048], P('ep', 'tp'), may hold values from -0.09375 to 0.09375
Outputs:
- result: bfloat16 [32, 2048], P('ep', 'tp')
- new_key: bfloat16 [32, 8, 256], P(('ep', 'tp'))
- new_value: bfloat16 [32, 8, 256], P(('ep', 'tp'))
The draws below stay inside these ranges and needn't reach their ends.
Inputs may be any that keep to these rules, and one draw needn't show every extreme that they name: `routes`: within the 4 rows of one index of ep no expert is named more than 4 times, and in some of them one expert is named exactly 4 times; the two experts of a row differ. `lengths`: every sequence has at least two live positions.
All inputs are finite; a program needn't handle non-finite values.
Results may differ from the reference program's by a relative error of at most 0.0099.
Values may be sent and summed in bfloat16 or wider, within the bound.
A program may use at most 64 MiB of HBM per device.

```python
import functools
import math
import jax
import jax.numpy as jnp
import numpy as np
from jax import lax

D = 2048
HEADS = 8
KVH = 8
DH = 128
VD = 256
QW = 2048
KW = 2048
VW = 2048
OW = 2048
FFE = 4096
CAP = 4
LEN = 224
GROUP = 4
SEQS = 32
EXPERTS = 8
N_EP = 8


def draw_cache_key(key, part):
    drawn = jnp.clip(1.75 * jax.random.normal(key, (SEQS, KVH, LEN, 2 * DH), jnp.float32), -12.0, 12.0)
    return drawn.astype(jnp.bfloat16)


def set_ends(drawn, key, low, top_value):
    shape = drawn.shape
    index_at = [jax.random.randint(jax.random.fold_in(key, axis), (), 0, shape[axis]) for axis in range(len(shape))]
    drawn = drawn.at[tuple(index_at)].set(low)
    longest = shape.index(max(shape))
    index_at[longest] = (index_at[longest] + 1) % shape[longest]
    return drawn.at[tuple(index_at)].set(top_value)


def levels(key, dims, cuts, least, largest):
    factor_of, own = 1.0, jax.random.fold_in(key, 6)
    for axis_at, blocks in cuts:
        steps = jnp.exp(jax.random.uniform(jax.random.fold_in(own, axis_at), (blocks,), jnp.float32, least / len(cuts), largest / len(cuts)))
        factor_of = factor_of * jnp.repeat(steps, dims[axis_at] // blocks).reshape([-1 if axis == axis_at else 1 for axis in range(len(dims))])
    return factor_of


def shared_out(own_key, own, number, rows, amount, top, bound, skew):
    ranking = jax.random.permutation(own_key, amount)
    heavy_load, common = portions_of(amount, rows * top, bound, skew, True), portions_of(amount, rows * top, bound, skew, False)
    places = jnp.arange(amount)

    def named(sizes, rotation):
        used = int((sizes > 0).sum())
        fixed = max(1, used // 4)
        shifted = fixed + (places - fixed + rotation * (used - fixed)) % max(1, amount - fixed)
        return jnp.zeros((amount,), jnp.int32).at[ranking[jnp.where(places < fixed, places, shifted)]].set(jnp.asarray(sizes, jnp.int32))

    sizes = jnp.where(number % 4 == 0, named(heavy_load, number // 4), named(common, number - number // 4 - 1))
    mixed = jax.random.permutation(jax.random.fold_in(own, 3), amount)
    giver, sink = mixed[0:amount // 2 * 2:2], mixed[1:amount // 2 * 2:2]
    slack = jnp.minimum(sizes[giver] - 1, bound - sizes[sink]) // 2
    slack = jnp.where((giver == ranking[0]) | (sink == ranking[0]) | (sizes[sink] == 0), 0, jnp.maximum(slack, 0))
    shifted = jax.random.randint(jax.random.fold_in(own, 4), (amount // 2,), 0, 1 << 20) % (slack + 1)
    sizes = sizes.at[giver].add(-shifted).at[sink].add(shifted)
    members = jnp.searchsorted(jnp.cumsum(sizes), jnp.arange(rows * top), side="right").astype(jnp.int32)
    listing = members.reshape(top, rows).T
    listing = listing[jax.random.permutation(jax.random.fold_in(own, 1), rows)]
    rotation = jax.random.randint(jax.random.fold_in(own, 2), (rows, 1), 0, top)
    return jnp.take_along_axis(listing, (jnp.arange(top)[None, :] + rotation) % top, axis=1)


def portions_of(amount, total, bound, slope, full):
    weights = [(1 << 20) // math.isqrt(grade ** slope) + 1 for grade in range(1, amount + 1)]
    largest = bound if full else min(bound, max(-(-total // amount), total * weights[0] // sum(weights)))
    least = 1 if total - largest >= amount - 1 else 0
    counts, rest = [largest] + [least] * (amount - 1), total - largest - least * (amount - 1)
    while rest > 0:
        candidates = [i for i in range(1, amount) if counts[i] < largest] or [i for i in range(1, amount) if counts[i] < bound]
        pool, remaining = sum([weights[i] for i in candidates]), rest
        for i in candidates:
            addition = min(bound - counts[i], max(1, remaining * weights[i] // pool), rest)
            counts[i] = counts[i] + addition
            rest = rest - addition
    return np.array(counts)


def gaussian(key, extent, deviation, reach, shards=(), held_as=jnp.bfloat16):
    values = deviation * jax.random.normal(key, extent, jnp.float32)
    if shards:
        values = values * levels(key, extent, shards, -0.22, 0.18)
    return jnp.clip(values, -reach, reach).astype(held_as)


def setup_inputs(seed: int = 0) -> dict:
    splits = jax.random.split(jax.random.key(seed), 20)
    resid = gaussian(splits[0], (SEQS, D), 1.0, 6.0, ((0, 8), (1, 4)))
    cache_key = draw_cache_key(jax.random.fold_in(splits[19], 71), 0)
    cache_value = gaussian(splits[2], (SEQS, KVH, LEN, VD), 1.0, 6.0, ((0, 32),))
    lengths = set_ends(jax.random.randint(splits[3], (SEQS,), LEN // 8, LEN + 1), jax.random.fold_in(splits[3], 1), LEN // 8, LEN).astype(jnp.int32)
    lambdas = jnp.clip(jax.random.uniform(splits[4], (HEADS,), jnp.float32, 0.3, 0.8), 0.3, 0.8)
    mix_gain = jnp.clip(1.0 + 0.18 * jax.random.normal(splits[5], (D,), jnp.float32), 0.1, 1.9)
    query_gain = jnp.clip(1.0 + 0.18 * jax.random.normal(splits[6], (DH,), jnp.float32), 0.1, 1.9)
    key_gain = jnp.clip(1.0 + 0.18 * jax.random.normal(splits[7], (DH,), jnp.float32), 0.1, 1.9)
    sub_gain = jnp.clip(1.0 + 0.18 * jax.random.normal(splits[8], (VD,), jnp.float32), 0.1, 1.9)
    ffn_gain = jnp.clip(1.0 + 0.18 * jax.random.normal(splits[9], (D,), jnp.float32), 0.1, 1.9)
    w_query = gaussian(splits[10], (D, QW), D ** -0.5, 0.125, ((1, 4),))
    w_key = gaussian(splits[11], (D, KW), D ** -0.5, 0.125, ((1, 4),))
    w_value = gaussian(splits[12], (D, VW), D ** -0.5, 0.125, ((1, 4),))
    w_out = gaussian(splits[13], (OW, D), OW ** -0.5, 0.125, ((1, 4),))
    routes_keys = jax.random.split(jax.random.fold_in(splits[14], 1), SEQS // GROUP)
    routes_turns = jax.random.permutation(jax.random.fold_in(splits[14], 3), SEQS // GROUP)
    routes = jax.vmap(lambda own, number: shared_out(jax.random.fold_in(splits[14], 2), own, number, GROUP, EXPERTS, 2, CAP, 2))(routes_keys, routes_turns).reshape((SEQS, 2))
    route_weights = jnp.clip(0.2 + 0.6 * jax.random.uniform(splits[15], (SEQS, 2), jnp.float32) ** levels(splits[15], (SEQS, 2), ((0, 8),), -0.2, 0.2), 0.2, 0.8)
    w_gate = gaussian(splits[16], (EXPERTS, D, FFE), D ** -0.5, 0.125, ((0, 8), (2, 4)))
    w_up = gaussian(splits[17], (EXPERTS, D, FFE), D ** -0.5, 0.125, ((0, 8), (2, 4)))
    w_down = gaussian(splits[18], (EXPERTS, FFE, D), FFE ** -0.5, 0.09375, ((0, 8), (1, 4)))
    return {"resid": resid, "cache_key": cache_key, "cache_value": cache_value, "lengths": lengths, "lambdas": lambdas, "mix_gain": mix_gain, "query_gain": query_gain, "key_gain": key_gain, "sub_gain": sub_gain, "ffn_gain": ffn_gain, "w_query": w_query, "w_key": w_key, "w_value": w_value, "w_out": w_out, "routes": routes, "route_weights": route_weights, "w_gate": w_gate, "w_up": w_up, "w_down": w_down}


epsilon = 1e-06
out_factor = 0.2 + 0.6 * math.exp(-0.3)
masked_score = -1e+30

def scaled_rows(values, gain):
    wide = values.astype(jnp.float32)
    return wide * lax.rsqrt(lax.optimization_barrier(jnp.mean(wide * wide, axis=-1, keepdims=True)) + epsilon) * gain

def route_tables(routes, route_weights, experts, capacity):
    flat_routes = routes.reshape(-1)
    expert_hit = (flat_routes[:, None] == jnp.arange(experts, dtype=jnp.int32)[None, :]).astype(jnp.int32)
    before = jnp.cumsum(expert_hit, axis=0) - expert_hit
    slot_index = lax.optimization_barrier(jnp.sum(before * expert_hit, axis=1))
    slot_hit = (slot_index[:, None] == jnp.arange(capacity, dtype=jnp.int32)[None, :]).astype(jnp.float32)
    pair_table = expert_hit.astype(jnp.float32)[:, :, None] * slot_hit[:, None, :]
    pair_table = pair_table.reshape(routes.shape[0], 2, experts, capacity)
    dispatch = lax.optimization_barrier(jnp.sum(pair_table, axis=1))
    combine = lax.optimization_barrier(jnp.sum(pair_table * route_weights[:, :, None, None], axis=1))
    return (dispatch, combine)

def attend(queries, key_rows, value_rows, past_keys, past_values, live_len, lambdas, query_gain, key_gain, sub_gain):
    seq_count, kv_heads, cache_len, key_width = past_keys.shape
    head_dim = key_width // 2
    head_count = lambdas.shape[0]
    group_size = head_count // kv_heads
    value_dim = past_values.shape[-1]
    score_scale = head_dim ** (-0.5)
    highest = lax.Precision.HIGHEST
    q_unit = scaled_rows(queries.reshape(seq_count, kv_heads, group_size, 2, head_dim), query_gain).astype(jnp.bfloat16)
    new_key = scaled_rows(key_rows.reshape(seq_count, kv_heads, 2, head_dim), key_gain).astype(jnp.bfloat16)
    new_value = value_rows.reshape(seq_count, kv_heads, value_dim)
    past_split = past_keys.reshape(seq_count, kv_heads, cache_len, 2, head_dim)
    scores = jnp.einsum('sjgmd,sjlmd->sjgml', q_unit.astype(jnp.float32), past_split.astype(jnp.float32), precision=highest) * score_scale
    own_score = jnp.einsum('sjgmd,sjmd->sjgm', q_unit.astype(jnp.float32), new_key.astype(jnp.float32), precision=highest) * score_scale
    live_mask = jnp.arange(cache_len, dtype=jnp.int32)[None, :] < live_len[:, None]
    scores = jnp.where(live_mask[:, None, None, None, :], scores, masked_score)
    peak = jnp.maximum(lax.optimization_barrier(jnp.max(scores, axis=-1)), own_score)
    past_weight = jnp.exp(scores - peak[..., None])
    own_weight = jnp.exp(own_score - peak)
    totals = lax.optimization_barrier(jnp.sum(past_weight, axis=-1)) + own_weight
    past_prob = past_weight / totals[..., None]
    own_prob = own_weight / totals
    mix_lambda = lambdas.reshape(1, kv_heads, group_size, 1)
    past_mix = (past_prob[..., 0, :] - mix_lambda * past_prob[..., 1, :]).astype(jnp.bfloat16)
    own_mix = (own_prob[..., 0] - mix_lambda[..., 0] * own_prob[..., 1]).astype(jnp.bfloat16)
    head_out = jnp.einsum('sjgl,sjlv->sjgv', past_mix.astype(jnp.float32), past_values.astype(jnp.float32), precision=highest)
    head_out = head_out + own_mix.astype(jnp.float32)[..., None] * new_value.astype(jnp.float32)[:, :, None, :]
    mixed = (scaled_rows(head_out, sub_gain) * out_factor).astype(jnp.bfloat16).reshape(seq_count, head_count * value_dim)
    return (mixed, new_key.reshape(seq_count, kv_heads, key_width), new_value)

def reference(resid, cache_key, cache_value, lengths, lambdas, mix_gain, query_gain, key_gain, sub_gain, ffn_gain, w_query, w_key, w_value, w_out, routes, route_weights, w_gate, w_up, w_down):
    normed = scaled_rows(resid, mix_gain).astype(jnp.bfloat16)
    queries = jnp.dot(normed, w_query, preferred_element_type=jnp.float32).astype(jnp.bfloat16)
    key_rows = jnp.dot(normed, w_key, preferred_element_type=jnp.float32).astype(jnp.bfloat16)
    value_rows = jnp.dot(normed, w_value, preferred_element_type=jnp.float32).astype(jnp.bfloat16)
    block_count = SEQS // GROUP

    def split_blocks(array):
        return array.reshape((block_count, GROUP) + array.shape[1:])

    def one_block(block_args):
        return attend(block_args[0], block_args[1], block_args[2], block_args[3], block_args[4], block_args[5], lambdas, query_gain, key_gain, sub_gain)
    mixed, new_key, new_value = lax.map(one_block, (split_blocks(queries), split_blocks(key_rows), split_blocks(value_rows), split_blocks(cache_key), split_blocks(cache_value), split_blocks(lengths)))
    mixed = mixed.reshape(SEQS, OW)
    updated = (resid.astype(jnp.float32) + jnp.dot(mixed, w_out, preferred_element_type=jnp.float32)).astype(jnp.bfloat16)
    hidden = scaled_rows(updated, ffn_gain).astype(jnp.bfloat16)
    tables = jax.vmap(functools.partial(route_tables, experts=EXPERTS, capacity=CAP))
    dispatch, combine = tables(routes.reshape(N_EP, GROUP, 2), route_weights.reshape(N_EP, GROUP, 2))
    highest = lax.Precision.HIGHEST
    send = jnp.einsum('ngec,ngd->encd', dispatch, hidden.reshape(N_EP, GROUP, D).astype(jnp.float32), precision=highest).astype(jnp.bfloat16)

    def one_expert(expert_args):
        gate_weight, up_weight, down_weight, slots = expert_args
        flat_rows = slots.reshape(N_EP * CAP, D)
        gate_out = jnp.dot(flat_rows, gate_weight, preferred_element_type=jnp.float32)
        up_out = jnp.dot(flat_rows, up_weight, preferred_element_type=jnp.float32)
        act = (jax.nn.silu(gate_out) * up_out).astype(jnp.bfloat16)
        return jnp.dot(act, down_weight, preferred_element_type=jnp.float32).reshape(N_EP, CAP, D)
    outputs = lax.map(one_expert, (w_gate, w_up, w_down, send))
    expert_mix = jnp.einsum('ngec,encd->ngd', combine, outputs, precision=highest).reshape(SEQS, D)
    result = (updated.astype(jnp.float32) + expert_mix).astype(jnp.bfloat16)
    return (result, new_key.reshape(SEQS, KVH, 2 * DH), new_value.reshape(SEQS, KVH, VD))
```

```python
import functools
import math

import jax
import jax.numpy as jnp
from jax import lax
from jax.experimental import pallas as pl
from jax.experimental.pallas import tpu as pltpu
from jax.sharding import PartitionSpec as P

CAP = 4


epsilon = 1e-06
out_factor = 0.2 + 0.6 * math.exp(-0.3)
masked_score = -1e30


def scaled_rows(values, gain):
    wide = values.astype(jnp.float32)
    return wide * lax.rsqrt(jnp.mean(wide * wide, axis=-1, keepdims=True) + epsilon) * gain


def route_tables(routes, route_weights, experts, capacity):
    flat_routes = routes.reshape(-1)
    expert_hit = (flat_routes[:, None] == jnp.arange(experts, dtype=jnp.int32)[None, :]).astype(
        jnp.int32
    )
    before = jnp.cumsum(expert_hit, axis=0) - expert_hit
    slot_index = jnp.sum(before * expert_hit, axis=1)
    slot_hit = (slot_index[:, None] == jnp.arange(capacity, dtype=jnp.int32)[None, :]).astype(
        jnp.float32
    )
    pair_table = expert_hit.astype(jnp.float32)[:, :, None] * slot_hit[:, None, :]
    pair_table = pair_table.reshape(routes.shape[0], 2, experts, capacity)
    dispatch = jnp.sum(pair_table, axis=1)
    combine = jnp.sum(pair_table * route_weights[:, :, None, None], axis=1)
    return (dispatch, combine)


def attend(
    queries,
    key_rows,
    value_rows,
    past_keys,
    past_values,
    live_len,
    lambdas,
    query_gain,
    key_gain,
    sub_gain,
):
    seq_count, kv_heads, cache_len, key_width = past_keys.shape
    head_dim = key_width // 2
    head_count = lambdas.shape[0]
    group_size = head_count // kv_heads
    value_dim = past_values.shape[-1]
    score_scale = head_dim ** (-0.5)
    q_unit = scaled_rows(
        queries.reshape(seq_count, kv_heads, group_size, 2, head_dim), query_gain
    ).astype(jnp.bfloat16)
    new_key = scaled_rows(key_rows.reshape(seq_count, kv_heads, 2, head_dim), key_gain).astype(
        jnp.bfloat16
    )
    new_value = value_rows.reshape(seq_count, kv_heads, value_dim)
    past_split = past_keys.reshape(seq_count, kv_heads, cache_len, 2, head_dim)
    scores = (
        jnp.einsum("sjgmd,sjlmd->sjgml", q_unit, past_split, preferred_element_type=jnp.float32)
        * score_scale
    )
    own_score = (
        jnp.einsum("sjgmd,sjmd->sjgm", q_unit, new_key, preferred_element_type=jnp.float32)
        * score_scale
    )
    live_mask = jnp.arange(cache_len, dtype=jnp.int32)[None, :] < live_len[:, None]
    scores = jnp.where(live_mask[:, None, None, None, :], scores, masked_score)
    peak = jnp.maximum(jnp.max(scores, axis=-1), own_score)
    past_weight = jnp.exp(scores - peak[..., None])
    own_weight = jnp.exp(own_score - peak)
    totals = jnp.sum(past_weight, axis=-1) + own_weight
    past_prob = past_weight / totals[..., None]
    own_prob = own_weight / totals
    mix_lambda = lambdas.reshape(1, kv_heads, group_size, 1)
    past_mix = (past_prob[..., 0, :] - mix_lambda * past_prob[..., 1, :]).astype(jnp.bfloat16)
    own_mix = (own_prob[..., 0] - mix_lambda[..., 0] * own_prob[..., 1]).astype(jnp.bfloat16)
    head_out = jnp.einsum(
        "sjgl,sjlv->sjgv", past_mix, past_values, preferred_element_type=jnp.float32
    )
    head_out = (
        head_out
        + own_mix.astype(jnp.float32)[..., None] * new_value.astype(jnp.float32)[:, :, None, :]
    )
    mixed = (
        (scaled_rows(head_out, sub_gain) * out_factor)
        .astype(jnp.bfloat16)
        .reshape(seq_count, head_count * value_dim)
    )
    return (mixed, new_key.reshape(seq_count, kv_heads, key_width), new_value)


def local(
    resid,
    cache_key,
    cache_value,
    lengths,
    lambdas,
    mix_gain,
    query_gain,
    key_gain,
    sub_gain,
    ffn_gain,
    w_query,
    w_key,
    w_value,
    w_out,
    routes,
    route_weights,
    w_gate,
    w_up,
    w_down,
):
    gathered = lax.all_gather(resid, "tp", axis=1, tiled=True)
    normed = scaled_rows(gathered, mix_gain).astype(jnp.bfloat16)
    query_part = jnp.dot(normed, w_query, preferred_element_type=jnp.float32).astype(jnp.bfloat16)
    key_part = jnp.dot(normed, w_key, preferred_element_type=jnp.float32).astype(jnp.bfloat16)
    value_part = jnp.dot(normed, w_value, preferred_element_type=jnp.float32).astype(jnp.bfloat16)
    queries, key_rows, value_rows = (
        lax.all_to_all(query_part, "tp", split_axis=0, concat_axis=1, tiled=True),
        lax.all_to_all(key_part, "tp", split_axis=0, concat_axis=1, tiled=True),
        lax.all_to_all(value_part, "tp", split_axis=0, concat_axis=1, tiled=True),
    )
    mixed, new_key, new_value = attend(
        queries,
        key_rows,
        value_rows,
        cache_key,
        cache_value,
        lengths,
        lambdas,
        query_gain,
        key_gain,
        sub_gain,
    )
    attn_proj = jnp.dot(
        lax.all_gather(mixed, "tp", axis=0, tiled=True), w_out, preferred_element_type=jnp.float32
    )
    updated = (resid.astype(jnp.float32) + attn_proj).astype(jnp.bfloat16)
    updated_rows = lax.all_gather(updated, "tp", axis=1, tiled=True)
    hidden = scaled_rows(updated_rows, ffn_gain).astype(jnp.bfloat16)
    experts = w_gate.shape[0] * lax.axis_size("ep")
    dispatch, combine = route_tables(routes, route_weights, experts, CAP)
    send = jnp.einsum(
        "gec,gd->ecd", dispatch.astype(jnp.bfloat16), hidden, preferred_element_type=jnp.float32
    ).astype(jnp.bfloat16)
    slots = lax.all_to_all(send, "ep", split_axis=0, concat_axis=0, tiled=True)
    flat_rows = slots.reshape(-1, slots.shape[-1])
    gate_out = jnp.dot(flat_rows, w_gate[0], preferred_element_type=jnp.float32)
    up_out = jnp.dot(flat_rows, w_up[0], preferred_element_type=jnp.float32)
    act = (jax.nn.silu(gate_out) * up_out).astype(jnp.bfloat16)
    down_out = jnp.dot(act, w_down[0], preferred_element_type=jnp.float32)
    partial_value = down_out.reshape(slots.shape[0], slots.shape[1], down_out.shape[-1])
    flat_combine = combine.reshape(combine.shape[0], -1)
    summed = lax.psum_scatter(
        partial_value.astype(jnp.bfloat16), "tp", scatter_dimension=2, tiled=True
    ).astype(jnp.float32)
    returned = lax.all_to_all(
        summed.astype(jnp.bfloat16), "ep", split_axis=0, concat_axis=0, tiled=True
    ).astype(summed.dtype)
    expert_mix = jnp.dot(
        flat_combine,
        returned.reshape(-1, returned.shape[-1]),
        precision=lax.Precision.HIGHEST,
        preferred_element_type=jnp.float32,
    )
    result = (updated.astype(jnp.float32) + expert_mix).astype(jnp.bfloat16)
    return (result, new_key, new_value)


MESH = pl.DeviceIdType.MESH


def rms_scale(wide):
    return lax.rsqrt(jnp.mean(wide * wide, axis=-1, keepdims=True) + epsilon)


def fused(
    n_ep,
    n_tp,
    lengths,
    lambdas,
    resid,
    mix_gain,
    query_gain,
    key_gain,
    sub_gain,
    ffn_gain,
    routes,
    route_weights,
    w_query,
    w_key,
    w_value,
    cache_key,
    cache_value,
    w_out,
    w_gate,
    w_up,
    w_down,
    result,
    new_key,
    new_value,
    mix_gain_v,
    query_gain_v,
    key_gain_v,
    sub_gain_v,
    ffn_gain_v,
    routes_v,
    weights_v,
    wq_v,
    wk_v,
    wv_v,
    ck_v,
    cv_v,
    wo_v,
    wg_v,
    wu_v,
    wd_v,
    res_all,
    proj_send,
    proj_all,
    heads_v,
    mix_all,
    upd_all,
    rows_v,
    part_send,
    part_all,
    result_v,
    new_key_v,
    new_value_v,
    load_sem,
    out_sem,
    res_s,
    res_r,
    proj_s,
    proj_r,
    mix_s,
    mix_r,
    upd_s,
    upd_r,
    part_s,
    part_r,
):
    f32, bf16 = jnp.float32, jnp.bfloat16
    ep, tp = lax.axis_index("ep"), lax.axis_index("tp")
    count = n_ep * n_tp
    me = ep * n_tp + tp
    group, width = resid.shape
    kv_heads, cache_len, key_width = ck_v.shape
    head_dim = key_width // 2
    heads_here = width // key_width

    loads = [
        (resid, res_all.at[tp]),
        (mix_gain, mix_gain_v),
        (w_query, wq_v),
        (w_key, wk_v),
        (w_value, wv_v),
        (query_gain, query_gain_v),
        (key_gain, key_gain_v),
        (sub_gain, sub_gain_v),
        (ffn_gain, ffn_gain_v),
        (routes, routes_v),
        (route_weights, weights_v),
        (cache_key.at[0], ck_v),
        (cache_value.at[0], cv_v),
        (w_out, wo_v),
        (w_gate.at[0], wg_v),
        (w_up.at[0], wu_v),
        (w_down.at[0], wd_v),
    ]
    copies = [
        pltpu.make_async_copy(source, target, load_sem.at[at])
        for at, (source, target) in enumerate(loads)
    ]
    for copy in copies:
        copy.start()
    (
        resid_c,
        mix_gain_c,
        wq_c,
        wk_c,
        wv_c,
        query_gain_c,
        key_gain_c,
        sub_gain_c,
        ffn_gain_c,
        routes_c,
        weights_c,
        ck_c,
        cv_c,
        wo_c,
        wg_c,
        wu_c,
        wd_c,
    ) = copies

    barrier = pltpu.get_barrier_semaphore()

    def greet(step, carry):
        other = lax.rem(me + step, count)
        pl.semaphore_signal(
            barrier,
            inc=1,
            device_id=(other // n_tp, lax.rem(other, n_tp)),
            device_id_type=MESH,
        )
        return carry

    lax.fori_loop(1, count, greet, 0)
    pl.semaphore_wait(barrier, count - 1)

    def tp_copy(step, source, target, send, recv):
        peer = lax.rem(tp + step, n_tp)
        return pltpu.make_async_remote_copy(
            src_ref=source(peer),
            dst_ref=target.at[tp],
            send_sem=send.at[step],
            recv_sem=recv.at[tp],
            device_id=(ep, peer),
            device_id_type=MESH,
        )

    def tp_wait(step, target, send, recv):
        peer = lax.rem(tp + step, n_tp)
        return pltpu.make_async_remote_copy(
            src_ref=target.at[peer],
            dst_ref=target.at[peer],
            send_sem=send.at[step],
            recv_sem=recv.at[peer],
            device_id=(ep, peer),
            device_id_type=MESH,
        )

    resid_c.wait()
    for step in range(1, n_tp):
        tp_copy(step, lambda peer: res_all.at[tp], res_all, res_s, res_r).start()
    mix_gain_c.wait()
    for step in range(1, n_tp):
        tp_wait(step, res_all, res_s, res_r).wait_recv()
    wide = jnp.concatenate([res_all[t].astype(f32) for t in range(n_tp)], axis=1)
    normed = (wide * rms_scale(wide) * mix_gain_v[...]).astype(bf16)

    blocks = 2 * heads_here
    for section, (copy, weight) in enumerate(((wq_c, wq_v), (wk_c, wk_v), (wv_c, wv_v))):
        copy.wait()
        out = jnp.dot(normed, weight[...], preferred_element_type=f32).astype(bf16).astype(f32)
        for head in range(heads_here):
            for half in range(2):
                at = (head * 2 + half) * head_dim
                proj_send[:, section * blocks + half * heads_here + head, :] = out[
                    :, at : at + head_dim
                ]
    for step in range(1, n_tp):
        tp_copy(step, lambda peer: proj_send.at[peer], proj_all, proj_s, proj_r).start()
    proj_all[tp] = proj_send[tp]
    for copy in (query_gain_c, key_gain_c, sub_gain_c, ffn_gain_c, routes_c, weights_c):
        copy.wait()
    for step in range(1, n_tp):
        tp_wait(step, proj_all, proj_s, proj_r).wait_recv()
    for t in range(n_tp):
        for section in range(3):
            for half in range(2):
                at = section * blocks + half * heads_here
                heads_v[section, half, t * heads_here : (t + 1) * heads_here, :] = proj_all[
                    t, at : at + heads_here, :
                ]
    maps = 2 * kv_heads
    q_raw = heads_v[0].reshape(maps, head_dim)
    k_raw = heads_v[1].reshape(maps, head_dim)
    q_unit = (q_raw * rms_scale(q_raw) * query_gain_v[...]).astype(bf16).astype(f32)
    k_unit = (k_raw * rms_scale(k_raw) * key_gain_v[...]).astype(bf16).astype(f32)
    value_own = jnp.concatenate([heads_v[2, 0], heads_v[2, 1]], axis=1)
    new_key_v[...] = jnp.concatenate([k_unit[:kv_heads], k_unit[kv_heads:]], axis=1).astype(bf16)
    new_value_v[...] = value_own.astype(bf16)
    out_copies = [
        pltpu.make_async_copy(new_key_v, new_key.at[0], out_sem.at[0]),
        pltpu.make_async_copy(new_value_v, new_value.at[0], out_sem.at[1]),
    ]
    for copy in out_copies:
        copy.start()

    row = lax.broadcasted_iota(jnp.int32, (maps, 1), 0)
    head_row = lax.rem(row, kv_heads)
    first = row < kv_heads
    q_wide = jnp.concatenate(
        [jnp.where(first, q_unit, 0.0), jnp.where(first, 0.0, q_unit)], axis=1
    ).astype(bf16)
    ck_c.wait()
    scores = jnp.zeros((maps, cache_len), f32)
    for head in range(kv_heads):
        part = lax.dot_general(
            q_wide, ck_v[head], (((1,), (1,)), ((), ())), preferred_element_type=f32
        )
        scores = jnp.where(head_row == head, part, scores)
    scale = head_dim ** (-0.5)
    own_score = jnp.sum(q_unit * k_unit, axis=-1, keepdims=True) * scale
    live = lax.broadcasted_iota(jnp.int32, (maps, cache_len), 1) < lengths[0]
    scores = jnp.where(live, scores * scale, masked_score)
    peak = jnp.maximum(jnp.max(scores, axis=-1, keepdims=True), own_score)
    past_weight = jnp.exp(scores - peak)
    own_weight = jnp.exp(own_score - peak)
    totals = jnp.sum(past_weight, axis=-1, keepdims=True) + own_weight
    past_prob = past_weight / totals
    own_prob = own_weight / totals
    lam = jnp.zeros((kv_heads, 1), f32)
    for head in range(kv_heads):
        lam = jnp.where(row[:kv_heads] == head, lambdas[head], lam)
    past_mix = (past_prob[:kv_heads] - lam * past_prob[kv_heads:]).astype(bf16)
    own_mix = (own_prob[:kv_heads] - lam * own_prob[kv_heads:]).astype(bf16).astype(f32)
    cv_c.wait()
    head_out = jnp.zeros((kv_heads, key_width), f32)
    for head in range(kv_heads):
        part = jnp.dot(past_mix, cv_v[head], preferred_element_type=f32)
        head_out = jnp.where(row[:kv_heads] == head, part, head_out)
    head_out = head_out + own_mix * value_own
    mixed = (head_out * rms_scale(head_out) * sub_gain_v[...] * out_factor).astype(bf16)
    mix_all[tp] = mixed.astype(f32)
    for step in range(1, n_tp):
        tp_copy(step, lambda peer: mix_all.at[tp], mix_all, mix_s, mix_r).start()
    wo_c.wait()
    for step in range(1, n_tp):
        tp_wait(step, mix_all, mix_s, mix_r).wait_recv()
    mixed_rows = jnp.concatenate([mix_all[:, head, :] for head in range(kv_heads)], axis=1)
    attn_proj = jnp.dot(mixed_rows.astype(bf16), wo_v[...], preferred_element_type=f32)
    updated = (res_all[tp].astype(f32) + attn_proj).astype(bf16)
    upd_all[me] = updated

    def any_copy(other, source, target, send, recv):
        return pltpu.make_async_remote_copy(
            src_ref=source,
            dst_ref=target.at[me],
            send_sem=send.at[other],
            recv_sem=recv.at[me],
            device_id=(other // n_tp, lax.rem(other, n_tp)),
            device_id_type=MESH,
        )

    def any_wait(other, target, send, recv):
        return pltpu.make_async_remote_copy(
            src_ref=target.at[other],
            dst_ref=target.at[other],
            send_sem=send.at[other],
            recv_sem=recv.at[other],
            device_id=(other // n_tp, lax.rem(other, n_tp)),
            device_id_type=MESH,
        )

    def upd_start(step, carry):
        any_copy(lax.rem(me + step, count), upd_all.at[me], upd_all, upd_s, upd_r).start()
        return carry

    lax.fori_loop(1, count, upd_start, 0)

    def upd_wait(step, carry):
        any_wait(lax.rem(me + step, count), upd_all, upd_s, upd_r).wait_recv()
        return carry

    wg_c.wait()
    wu_c.wait()
    wd_c.wait()
    lax.fori_loop(1, count, upd_wait, 0)
    for e in range(n_ep):
        for t in range(n_tp):
            rows_v[e * group : (e + 1) * group, t * width : (t + 1) * width] = upd_all[
                e * n_tp + t
            ].astype(f32)
    rows = rows_v[...]
    hidden = (rows * rms_scale(rows) * ffn_gain_v[...]).astype(bf16)
    gate_out = jnp.dot(hidden, wg_v[...], preferred_element_type=f32)
    up_out = jnp.dot(hidden, wu_v[...], preferred_element_type=f32)
    act = (jax.nn.silu(gate_out) * up_out).astype(bf16)

    for t in range(n_tp):
        slab = jnp.dot(act, wd_v[:, t * width : (t + 1) * width], preferred_element_type=f32)
        for e in range(n_ep):
            part_send[e * n_tp + t] = slab[e * group : (e + 1) * group].astype(bf16)

        def part_start(step, carry):
            other = lax.rem(ep + step, n_ep) * n_tp + t

            @pl.when(other != me)
            def _():
                any_copy(other, part_send.at[other], part_all, part_s, part_r).start()

            return carry

        lax.fori_loop(0, n_ep, part_start, 0)
    part_all[me] = part_send[me]

    def part_wait(step, carry):
        any_wait(lax.rem(me + step, count), part_all, part_s, part_r).wait_recv()
        return carry

    lax.fori_loop(1, count, part_wait, 0)
    expert_mix = jnp.zeros((group, width), f32)
    for e in range(n_ep):
        term = part_all[e * n_tp].astype(f32)
        for t in range(1, n_tp):
            term = term + part_all[e * n_tp + t].astype(f32)
        share = jnp.sum(jnp.where(routes_v[...] == e, weights_v[...], 0.0), axis=1, keepdims=True)
        expert_mix = expert_mix + share * term
    result_v[...] = (upd_all[me].astype(f32) + expert_mix).astype(bf16)
    out_copies.append(pltpu.make_async_copy(result_v, result, out_sem.at[2]))
    out_copies[2].start()

    for step in range(1, n_tp):
        tp_wait(step, res_all, res_s, res_r).wait_send()
        tp_wait(step, proj_all, proj_s, proj_r).wait_send()
        tp_wait(step, mix_all, mix_s, mix_r).wait_send()

    def drain(step, carry):
        other = lax.rem(me + step, count)
        any_wait(other, upd_all, upd_s, upd_r).wait_send()
        any_wait(other, part_all, part_s, part_r).wait_send()
        return carry

    lax.fori_loop(1, count, drain, 0)
    for copy in out_copies:
        copy.wait()


def fused_layer(n_ep, n_tp, *args):
    (
        resid,
        cache_key,
        cache_value,
        lengths,
        lambdas,
        mix_gain,
        query_gain,
        key_gain,
        sub_gain,
        ffn_gain,
        w_query,
        w_key,
        w_value,
        w_out,
        routes,
        route_weights,
        w_gate,
        w_up,
        w_down,
    ) = args
    bf16, f32 = jnp.bfloat16, jnp.float32
    group, width = resid.shape
    _, kv_heads, cache_len, key_width = cache_key.shape
    head_dim = key_width // 2
    features = width * n_tp
    hidden_units = w_gate.shape[2]
    count = n_ep * n_tp
    blocks = 6 * (width // key_width)
    any_spec = pl.BlockSpec(memory_space=pl.ANY)
    smem_spec = pl.BlockSpec(memory_space=pltpu.SMEM)
    operands = (
        lengths,
        lambdas,
        resid,
        mix_gain.reshape(1, -1),
        query_gain.reshape(1, -1),
        key_gain.reshape(1, -1),
        sub_gain.reshape(1, -1),
        ffn_gain.reshape(1, -1),
        routes,
        route_weights,
        w_query,
        w_key,
        w_value,
        cache_key,
        cache_value,
        w_out,
        w_gate,
        w_up,
        w_down,
    )
    dma = pltpu.SemaphoreType.DMA
    return pl.pallas_call(
        functools.partial(fused, n_ep, n_tp),
        out_shape=(
            jax.ShapeDtypeStruct((group, width), bf16),
            jax.ShapeDtypeStruct((1, kv_heads, key_width), bf16),
            jax.ShapeDtypeStruct((1, kv_heads, key_width), bf16),
        ),
        in_specs=[smem_spec] * 2 + [any_spec] * (len(operands) - 2),
        out_specs=(any_spec,) * 3,
        scratch_shapes=[
            pltpu.VMEM((1, features), f32),
            pltpu.VMEM((1, head_dim), f32),
            pltpu.VMEM((1, head_dim), f32),
            pltpu.VMEM((1, key_width), f32),
            pltpu.VMEM((1, features), f32),
            pltpu.VMEM(routes.shape, jnp.int32),
            pltpu.VMEM(routes.shape, f32),
            pltpu.VMEM((features, width), bf16),
            pltpu.VMEM((features, width), bf16),
            pltpu.VMEM((features, width), bf16),
            pltpu.VMEM((kv_heads, cache_len, key_width), bf16),
            pltpu.VMEM((kv_heads, cache_len, key_width), bf16),
            pltpu.VMEM((features, width), bf16),
            pltpu.VMEM((features, hidden_units), bf16),
            pltpu.VMEM((features, hidden_units), bf16),
            pltpu.VMEM((hidden_units, features), bf16),
            pltpu.VMEM((n_tp, group, width), bf16),
            pltpu.VMEM((n_tp, blocks, head_dim), f32),
            pltpu.VMEM((n_tp, blocks, head_dim), f32),
            pltpu.VMEM((3, 2, kv_heads, head_dim), f32),
            pltpu.VMEM((n_tp, kv_heads, key_width), f32),
            pltpu.VMEM((count, group, width), bf16),
            pltpu.VMEM((n_ep * group, features), f32),
            pltpu.VMEM((count, group, width), bf16),
            pltpu.VMEM((count, group, width), bf16),
            pltpu.VMEM((group, width), bf16),
            pltpu.VMEM((kv_heads, key_width), bf16),
            pltpu.VMEM((kv_heads, key_width), bf16),
            dma((17,)),
            dma((3,)),
        ]
        + [dma((n_tp,))] * 6
        + [dma((count,))] * 4,
        compiler_params=pltpu.CompilerParams(
            collective_id=0, has_side_effects=True, vmem_limit_bytes=60 * 1024 * 1024
        ),
        name="fused_layer",
    )(*operands)


def layer(n_ep, n_tp, *args):
    resid, cache_key, lambdas, w_gate = args[0], args[1], args[4], args[16]
    group, width = resid.shape
    sequences, kv_heads, _, key_width = cache_key.shape
    aligned = (
        sequences == 1
        and group == n_tp
        and n_tp > 1
        and lambdas.shape[0] == kv_heads
        and kv_heads % 8 == 0
        and key_width % 256 == 0
        and width % key_width == 0
        and w_gate.shape[0] == 1
        and n_ep * n_tp <= 32
    )
    if aligned:
        return fused_layer(n_ep, n_tp, *args)
    return local(*args)


def solution(mesh):
    in_specs = (
        P("ep", "tp"),
        P(("ep", "tp"), None, None, None),
        P(("ep", "tp"), None, None, None),
        P(("ep", "tp")),
        P(),
        P(),
        P(),
        P(),
        P(),
        P(),
        P(None, "tp"),
        P(None, "tp"),
        P(None, "tp"),
        P(None, "tp"),
        P("ep", None),
        P("ep", None),
        P("ep", None, "tp"),
        P("ep", None, "tp"),
        P("ep", "tp", None),
    )
    out_specs = (P("ep", "tp"), P(("ep", "tp"), None, None), P(("ep", "tp"), None, None))
    return jax.shard_map(functools.partial(layer, mesh.shape["ep"], mesh.shape["tp"]), mesh=mesh, in_specs=in_specs, out_specs=out_specs, check_vma=False)
```

```python
import functools
import math

import jax
import jax.numpy as jnp
from jax import lax
from jax.experimental import pallas as pl
from jax.experimental.pallas import tpu as pltpu
from jax.sharding import PartitionSpec as P

CAP = 4


epsilon = 1e-06
out_factor = 0.2 + 0.6 * math.exp(-0.3)
masked_score = -1e30


def scaled_rows(values, gain):
    wide = values.astype(jnp.float32)
    return wide * lax.rsqrt(jnp.mean(wide * wide, axis=-1, keepdims=True) + epsilon) * gain


def route_tables(routes, route_weights, experts, capacity):
    flat_routes = routes.reshape(-1)
    expert_hit = (flat_routes[:, None] == jnp.arange(experts, dtype=jnp.int32)[None, :]).astype(
        jnp.int32
    )
    before = jnp.cumsum(expert_hit, axis=0) - expert_hit
    slot_index = jnp.sum(before * expert_hit, axis=1)
    slot_hit = (slot_index[:, None] == jnp.arange(capacity, dtype=jnp.int32)[None, :]).astype(
        jnp.float32
    )
    pair_table = expert_hit.astype(jnp.float32)[:, :, None] * slot_hit[:, None, :]
    pair_table = pair_table.reshape(routes.shape[0], 2, experts, capacity)
    dispatch = jnp.sum(pair_table, axis=1)
    combine = jnp.sum(pair_table * route_weights[:, :, None, None], axis=1)
    return (dispatch, combine)


def attend(
    queries,
    key_rows,
    value_rows,
    past_keys,
    past_values,
    live_len,
    lambdas,
    query_gain,
    key_gain,
    sub_gain,
):
    seq_count, kv_heads, cache_len, key_width = past_keys.shape
    head_dim = key_width // 2
    head_count = lambdas.shape[0]
    group_size = head_count // kv_heads
    value_dim = past_values.shape[-1]
    score_scale = head_dim ** (-0.5)
    q_unit = scaled_rows(
        queries.reshape(seq_count, kv_heads, group_size, 2, head_dim), query_gain
    ).astype(jnp.bfloat16)
    new_key = scaled_rows(key_rows.reshape(seq_count, kv_heads, 2, head_dim), key_gain).astype(
        jnp.bfloat16
    )
    new_value = value_rows.reshape(seq_count, kv_heads, value_dim)
    past_split = past_keys.reshape(seq_count, kv_heads, cache_len, 2, head_dim)
    scores = (
        jnp.einsum("sjgmd,sjlmd->sjgml", q_unit, past_split, preferred_element_type=jnp.float32)
        * score_scale
    )
    own_score = (
        jnp.einsum("sjgmd,sjmd->sjgm", q_unit, new_key, preferred_element_type=jnp.float32)
        * score_scale
    )
    live_mask = jnp.arange(cache_len, dtype=jnp.int32)[None, :] < live_len[:, None]
    scores = jnp.where(live_mask[:, None, None, None, :], scores, masked_score)
    peak = jnp.maximum(jnp.max(scores, axis=-1), own_score)
    past_weight = jnp.exp(scores - peak[..., None])
    own_weight = jnp.exp(own_score - peak)
    totals = jnp.sum(past_weight, axis=-1) + own_weight
    past_prob = past_weight / totals[..., None]
    own_prob = own_weight / totals
    mix_lambda = lambdas.reshape(1, kv_heads, group_size, 1)
    past_mix = (past_prob[..., 0, :] - mix_lambda * past_prob[..., 1, :]).astype(jnp.bfloat16)
    own_mix = (own_prob[..., 0] - mix_lambda[..., 0] * own_prob[..., 1]).astype(jnp.bfloat16)
    head_out = jnp.einsum(
        "sjgl,sjlv->sjgv", past_mix, past_values, preferred_element_type=jnp.float32
    )
    head_out = (
        head_out
        + own_mix.astype(jnp.float32)[..., None] * new_value.astype(jnp.float32)[:, :, None, :]
    )
    mixed = (
        (scaled_rows(head_out, sub_gain) * out_factor)
        .astype(jnp.bfloat16)
        .reshape(seq_count, head_count * value_dim)
    )
    return (mixed, new_key.reshape(seq_count, kv_heads, key_width), new_value)


def local(
    resid,
    cache_key,
    cache_value,
    lengths,
    lambdas,
    mix_gain,
    query_gain,
    key_gain,
    sub_gain,
    ffn_gain,
    w_query,
    w_key,
    w_value,
    w_out,
    routes,
    route_weights,
    w_gate,
    w_up,
    w_down,
):
    gathered = lax.all_gather(resid, "tp", axis=1, tiled=True)
    normed = scaled_rows(gathered, mix_gain).astype(jnp.bfloat16)
    query_part = jnp.dot(normed, w_query, preferred_element_type=jnp.float32).astype(jnp.bfloat16)
    key_part = jnp.dot(normed, w_key, preferred_element_type=jnp.float32).astype(jnp.bfloat16)
    value_part = jnp.dot(normed, w_value, preferred_element_type=jnp.float32).astype(jnp.bfloat16)
    queries, key_rows, value_rows = (
        lax.all_to_all(query_part, "tp", split_axis=0, concat_axis=1, tiled=True),
        lax.all_to_all(key_part, "tp", split_axis=0, concat_axis=1, tiled=True),
        lax.all_to_all(value_part, "tp", split_axis=0, concat_axis=1, tiled=True),
    )
    mixed, new_key, new_value = attend(
        queries,
        key_rows,
        value_rows,
        cache_key,
        cache_value,
        lengths,
        lambdas,
        query_gain,
        key_gain,
        sub_gain,
    )
    attn_proj = jnp.dot(
        lax.all_gather(mixed, "tp", axis=0, tiled=True), w_out, preferred_element_type=jnp.float32
    )
    updated = (resid.astype(jnp.float32) + attn_proj).astype(jnp.bfloat16)
    updated_rows = lax.all_gather(updated, "tp", axis=1, tiled=True)
    hidden = scaled_rows(updated_rows, ffn_gain).astype(jnp.bfloat16)
    experts = w_gate.shape[0] * lax.axis_size("ep")
    dispatch, combine = route_tables(routes, route_weights, experts, CAP)
    send = jnp.einsum(
        "gec,gd->ecd", dispatch.astype(jnp.bfloat16), hidden, preferred_element_type=jnp.float32
    ).astype(jnp.bfloat16)
    slots = lax.all_to_all(send, "ep", split_axis=0, concat_axis=0, tiled=True)
    flat_rows = slots.reshape(-1, slots.shape[-1])
    gate_out = jnp.dot(flat_rows, w_gate[0], preferred_element_type=jnp.float32)
    up_out = jnp.dot(flat_rows, w_up[0], preferred_element_type=jnp.float32)
    act = (jax.nn.silu(gate_out) * up_out).astype(jnp.bfloat16)
    down_out = jnp.dot(act, w_down[0], preferred_element_type=jnp.float32)
    partial_value = down_out.reshape(slots.shape[0], slots.shape[1], down_out.shape[-1])
    flat_combine = combine.reshape(combine.shape[0], -1)
    summed = lax.psum_scatter(
        partial_value.astype(jnp.bfloat16), "tp", scatter_dimension=2, tiled=True
    ).astype(jnp.float32)
    returned = lax.all_to_all(
        summed.astype(jnp.bfloat16), "ep", split_axis=0, concat_axis=0, tiled=True
    ).astype(summed.dtype)
    expert_mix = jnp.dot(
        flat_combine,
        returned.reshape(-1, returned.shape[-1]),
        precision=lax.Precision.HIGHEST,
        preferred_element_type=jnp.float32,
    )
    result = (updated.astype(jnp.float32) + expert_mix).astype(jnp.bfloat16)
    return (result, new_key, new_value)


MESH = pl.DeviceIdType.MESH


def rms_scale(wide):
    return lax.rsqrt(jnp.mean(wide * wide, axis=-1, keepdims=True) + epsilon)


def fused(
    n_ep,
    n_tp,
    lengths,
    lambdas,
    resid,
    mix_gain,
    query_gain,
    key_gain,
    sub_gain,
    ffn_gain,
    routes,
    route_weights,
    w_query,
    w_key,
    w_value,
    cache_key,
    cache_value,
    w_out,
    w_gate,
    w_up,
    w_down,
    result,
    new_key,
    new_value,
    mix_gain_v,
    query_gain_v,
    key_gain_v,
    sub_gain_v,
    ffn_gain_v,
    lengths_v,
    lambdas_v,
    routes_v,
    weights_v,
    wq_v,
    wk_v,
    wv_v,
    ck_v,
    cv_v,
    wo_v,
    wg_v,
    wu_v,
    wd_v,
    res_all,
    proj_send,
    proj_all,
    heads_v,
    mix_all,
    upd_all,
    rows_v,
    part_send,
    part_all,
    result_v,
    new_key_v,
    new_value_v,
    load_sem,
    out_sem,
    res_s,
    res_r,
    proj_s,
    proj_r,
    mix_s,
    mix_r,
    upd_s,
    upd_r,
    part_s,
    part_r,
):
    f32, bf16 = jnp.float32, jnp.bfloat16
    ep, tp = lax.axis_index("ep"), lax.axis_index("tp")
    count = n_ep * n_tp
    me = ep * n_tp + tp
    group, width = resid.shape
    kv_heads, cache_len, key_width = ck_v.shape
    head_dim = key_width // 2
    heads_here = width // key_width

    loads = [
        (resid, res_all.at[tp]),
        (mix_gain, mix_gain_v),
        (w_query, wq_v),
        (w_key, wk_v),
        (w_value, wv_v),
        (query_gain, query_gain_v),
        (key_gain, key_gain_v),
        (sub_gain, sub_gain_v),
        (ffn_gain, ffn_gain_v),
        (lengths, lengths_v),
        (lambdas, lambdas_v),
        (routes, routes_v),
        (route_weights, weights_v),
        (cache_key.at[0], ck_v),
        (cache_value.at[0], cv_v),
        (w_out, wo_v),
        (w_gate.at[0], wg_v),
        (w_up.at[0], wu_v),
        (w_down.at[0], wd_v),
    ]
    copies = [
        pltpu.make_async_copy(source, target, load_sem.at[at])
        for at, (source, target) in enumerate(loads)
    ]
    for copy in copies[:5]:
        copy.start()
    (
        resid_c,
        mix_gain_c,
        wq_c,
        wk_c,
        wv_c,
        query_gain_c,
        key_gain_c,
        sub_gain_c,
        ffn_gain_c,
        lengths_c,
        lambdas_c,
        routes_c,
        weights_c,
        ck_c,
        cv_c,
        wo_c,
        wg_c,
        wu_c,
        wd_c,
    ) = copies

    barrier = pltpu.get_barrier_semaphore()

    for step in range(1, n_tp):
        pl.semaphore_signal(
            barrier, inc=1, device_id=(ep, lax.rem(tp + step, n_tp)), device_id_type=MESH
        )
    for step in range(1, n_ep):
        pl.semaphore_signal(
            barrier, inc=1, device_id=(lax.rem(ep + step, n_ep), tp), device_id_type=MESH
        )
    for copy in copies[5:]:
        copy.start()
    pl.semaphore_wait(barrier, n_tp + n_ep - 2)

    def tp_copy(step, source, target, send, recv):
        peer = lax.rem(tp + step, n_tp)
        return pltpu.make_async_remote_copy(
            src_ref=source(peer),
            dst_ref=target.at[tp],
            send_sem=send.at[step],
            recv_sem=recv.at[tp],
            device_id=(ep, peer),
            device_id_type=MESH,
        )

    def tp_wait(step, target, send, recv):
        peer = lax.rem(tp + step, n_tp)
        return pltpu.make_async_remote_copy(
            src_ref=target.at[peer],
            dst_ref=target.at[peer],
            send_sem=send.at[step],
            recv_sem=recv.at[peer],
            device_id=(ep, peer),
            device_id_type=MESH,
        )

    resid_c.wait()
    for step in range(1, n_tp):
        tp_copy(step, lambda peer: res_all.at[tp], res_all, res_s, res_r).start()
    mix_gain_c.wait()
    for step in range(1, n_tp):
        tp_wait(step, res_all, res_s, res_r).wait_recv()
    wide = jnp.concatenate([res_all[t].astype(f32) for t in range(n_tp)], axis=1)
    normed = (wide * rms_scale(wide) * mix_gain_v[...]).astype(bf16)

    blocks = 2 * heads_here
    for section, (copy, weight) in enumerate(((wq_c, wq_v), (wk_c, wk_v), (wv_c, wv_v))):
        copy.wait()
        out = jnp.dot(normed, weight[...], preferred_element_type=f32).astype(bf16).astype(f32)
        for head in range(heads_here):
            for half in range(2):
                at = (head * 2 + half) * head_dim
                proj_send[:, section * blocks + half * heads_here + head, :] = out[
                    :, at : at + head_dim
                ]
    for step in range(1, n_tp):
        tp_copy(step, lambda peer: proj_send.at[peer], proj_all, proj_s, proj_r).start()
    proj_all[tp] = proj_send[tp]
    for copy in (query_gain_c, key_gain_c, sub_gain_c, ffn_gain_c, lengths_c, lambdas_c, routes_c, weights_c):
        copy.wait()
    for step in range(1, n_tp):
        tp_wait(step, proj_all, proj_s, proj_r).wait_recv()
    for t in range(n_tp):
        for section in range(3):
            for half in range(2):
                at = section * blocks + half * heads_here
                heads_v[section, half, t * heads_here : (t + 1) * heads_here, :] = proj_all[
                    t, at : at + heads_here, :
                ]
    maps = 2 * kv_heads
    q_raw = heads_v[0].reshape(maps, head_dim)
    k_raw = heads_v[1].reshape(maps, head_dim)
    q_unit = (q_raw * rms_scale(q_raw) * query_gain_v[...]).astype(bf16).astype(f32)
    k_unit = (k_raw * rms_scale(k_raw) * key_gain_v[...]).astype(bf16).astype(f32)
    value_own = jnp.concatenate([heads_v[2, 0], heads_v[2, 1]], axis=1)
    new_key_v[...] = jnp.concatenate([k_unit[:kv_heads], k_unit[kv_heads:]], axis=1).astype(bf16)
    new_value_v[...] = value_own.astype(bf16)
    out_copies = [
        pltpu.make_async_copy(new_key_v, new_key.at[0], out_sem.at[0]),
        pltpu.make_async_copy(new_value_v, new_value.at[0], out_sem.at[1]),
    ]
    for copy in out_copies:
        copy.start()

    row = lax.broadcasted_iota(jnp.int32, (maps, 1), 0)
    head_row = lax.rem(row, kv_heads)
    first = row < kv_heads
    q_wide = jnp.concatenate(
        [jnp.where(first, q_unit, 0.0), jnp.where(first, 0.0, q_unit)], axis=1
    ).astype(bf16)
    ck_c.wait()
    scores = jnp.zeros((maps, cache_len), f32)
    for head in range(kv_heads):
        part = lax.dot_general(
            q_wide, ck_v[head], (((1,), (1,)), ((), ())), preferred_element_type=f32
        )
        scores = jnp.where(head_row == head, part, scores)
    scale = head_dim ** (-0.5)
    own_score = jnp.sum(q_unit * k_unit, axis=-1, keepdims=True) * scale
    live = lax.broadcasted_iota(jnp.int32, (maps, cache_len), 1) < lengths_v[0]
    scores = jnp.where(live, scores * scale, masked_score)
    peak = jnp.maximum(jnp.max(scores, axis=-1, keepdims=True), own_score)
    past_weight = jnp.exp(scores - peak)
    own_weight = jnp.exp(own_score - peak)
    totals = jnp.sum(past_weight, axis=-1, keepdims=True) + own_weight
    past_prob = past_weight / totals
    own_prob = own_weight / totals
    lam = jnp.zeros((kv_heads, 1), f32)
    for head in range(kv_heads):
        lam = jnp.where(row[:kv_heads] == head, lambdas_v[head], lam)
    past_mix = (past_prob[:kv_heads] - lam * past_prob[kv_heads:]).astype(bf16)
    own_mix = (own_prob[:kv_heads] - lam * own_prob[kv_heads:]).astype(bf16).astype(f32)
    cv_c.wait()
    head_out = jnp.zeros((kv_heads, key_width), f32)
    for head in range(kv_heads):
        part = jnp.dot(past_mix, cv_v[head], preferred_element_type=f32)
        head_out = jnp.where(row[:kv_heads] == head, part, head_out)
    head_out = head_out + own_mix * value_own
    mixed = (head_out * rms_scale(head_out) * sub_gain_v[...] * out_factor).astype(bf16)
    mix_all[tp] = mixed.astype(f32)
    for step in range(1, n_tp):
        tp_copy(step, lambda peer: mix_all.at[tp], mix_all, mix_s, mix_r).start()
    wo_c.wait()
    for step in range(1, n_tp):
        tp_wait(step, mix_all, mix_s, mix_r).wait_recv()
    mixed_rows = jnp.concatenate([mix_all[:, head, :] for head in range(kv_heads)], axis=1)
    attn_proj = jnp.dot(mixed_rows.astype(bf16), wo_v[...], preferred_element_type=f32)
    updated = (res_all[tp].astype(f32) + attn_proj).astype(bf16)
    upd_all[me] = updated

    token = lax.broadcasted_iota(jnp.int32, (group, 128), 0)
    expert = lax.broadcasted_iota(jnp.int32, (group, 128), 1)
    shares = jnp.zeros((group, 128), f32)
    for s in range(group):
        for k in range(2):
            named = jnp.logical_and(token == s, expert == routes_v[k, s])
            shares = jnp.where(named, weights_v[k, s], shares)

    def any_copy(other, source, target, send, recv):
        return pltpu.make_async_remote_copy(
            src_ref=source,
            dst_ref=target.at[me],
            send_sem=send,
            recv_sem=recv,
            device_id=(other // n_tp, lax.rem(other, n_tp)),
            device_id_type=MESH,
        )

    def any_wait(target, send, recv):
        span = target.at[pl.ds(0, count - 1)]
        return pltpu.make_async_remote_copy(
            src_ref=span,
            dst_ref=span,
            send_sem=send,
            recv_sem=recv,
            device_id=(ep, tp),
            device_id_type=MESH,
        )

    def upd_start(step, carry):
        any_copy(lax.rem(me + step, count), upd_all.at[me], upd_all, upd_s, upd_r).start()
        return carry

    lax.fori_loop(1, count, upd_start, 0)

    wg_c.wait()
    wu_c.wait()
    wd_c.wait()
    any_wait(upd_all, upd_s, upd_r).wait_recv()
    for e in range(n_ep):
        for t in range(n_tp):
            rows_v[e * group : (e + 1) * group, t * width : (t + 1) * width] = upd_all[
                e * n_tp + t
            ].astype(f32)
    rows = rows_v[...]
    hidden = (rows * rms_scale(rows) * ffn_gain_v[...]).astype(bf16)
    gate_out = jnp.dot(hidden, wg_v[...], preferred_element_type=f32)
    up_out = jnp.dot(hidden, wu_v[...], preferred_element_type=f32)
    act = (jax.nn.silu(gate_out) * up_out).astype(bf16)

    for t in range(n_tp):
        slab = jnp.dot(act, wd_v[:, t * width : (t + 1) * width], preferred_element_type=f32)
        for e in range(n_ep):
            part_send[e * n_tp + t] = slab[e * group : (e + 1) * group].astype(bf16)

        def part_start(step, carry):
            other = lax.rem(ep + step, n_ep) * n_tp + t

            @pl.when(other != me)
            def _():
                any_copy(other, part_send.at[other], part_all, part_s, part_r).start()

            return carry

        lax.fori_loop(0, n_ep, part_start, 0)
    part_all[me] = part_send[me]

    any_wait(part_all, part_s, part_r).wait_recv()
    expert_mix = jnp.zeros((group, width), f32)
    for e in range(n_ep):
        term = part_all[e * n_tp].astype(f32)
        for t in range(1, n_tp):
            term = term + part_all[e * n_tp + t].astype(f32)
        expert_mix = expert_mix + shares[:, e : e + 1] * term
    result_v[...] = (upd_all[me].astype(f32) + expert_mix).astype(bf16)
    out_copies.append(pltpu.make_async_copy(result_v, result, out_sem.at[2]))
    out_copies[2].start()

    for step in range(1, n_tp):
        tp_wait(step, res_all, res_s, res_r).wait_send()
        tp_wait(step, proj_all, proj_s, proj_r).wait_send()
        tp_wait(step, mix_all, mix_s, mix_r).wait_send()

    any_wait(upd_all, upd_s, upd_r).wait_send()
    any_wait(part_all, part_s, part_r).wait_send()
    for copy in out_copies:
        copy.wait()


def hand_over(*refs):
    for source, target in zip(refs[:3], refs[3:]):
        target[...] = source[...]


def fused_layer(n_ep, n_tp, *args):
    (
        resid,
        cache_key,
        cache_value,
        lengths,
        lambdas,
        mix_gain,
        query_gain,
        key_gain,
        sub_gain,
        ffn_gain,
        w_query,
        w_key,
        w_value,
        w_out,
        routes,
        route_weights,
        w_gate,
        w_up,
        w_down,
    ) = args
    bf16, f32 = jnp.bfloat16, jnp.float32
    group, width = resid.shape
    _, kv_heads, cache_len, key_width = cache_key.shape
    head_dim = key_width // 2
    features = width * n_tp
    hidden_units = w_gate.shape[2]
    count = n_ep * n_tp
    blocks = 6 * (width // key_width)
    any_spec = pl.BlockSpec(memory_space=pl.ANY)
    operands = (
        lengths,
        lambdas,
        resid,
        mix_gain.reshape(1, -1),
        query_gain.reshape(1, -1),
        key_gain.reshape(1, -1),
        sub_gain.reshape(1, -1),
        ffn_gain.reshape(1, -1),
        routes.T,
        route_weights.T,
        w_query,
        w_key,
        w_value,
        cache_key,
        cache_value,
        w_out,
        w_gate,
        w_up,
        w_down,
    )
    dma = pltpu.SemaphoreType.DMA
    outs = pl.pallas_call(
        functools.partial(fused, n_ep, n_tp),
        out_shape=(
            jax.ShapeDtypeStruct((group, width), bf16),
            jax.ShapeDtypeStruct((1, kv_heads, key_width), bf16),
            jax.ShapeDtypeStruct((1, kv_heads, key_width), bf16),
        ),
        in_specs=[any_spec] * len(operands),
        out_specs=(any_spec,) * 3,
        scratch_shapes=[
            pltpu.VMEM((1, features), f32),
            pltpu.VMEM((1, head_dim), f32),
            pltpu.VMEM((1, head_dim), f32),
            pltpu.VMEM((1, key_width), f32),
            pltpu.VMEM((1, features), f32),
            pltpu.SMEM(lengths.shape, jnp.int32),
            pltpu.SMEM(lambdas.shape, f32),
            pltpu.SMEM(routes.shape[::-1], jnp.int32),
            pltpu.SMEM(routes.shape[::-1], f32),
            pltpu.VMEM((features, width), bf16),
            pltpu.VMEM((features, width), bf16),
            pltpu.VMEM((features, width), bf16),
            pltpu.VMEM((kv_heads, cache_len, key_width), bf16),
            pltpu.VMEM((kv_heads, cache_len, key_width), bf16),
            pltpu.VMEM((features, width), bf16),
            pltpu.VMEM((features, hidden_units), bf16),
            pltpu.VMEM((features, hidden_units), bf16),
            pltpu.VMEM((hidden_units, features), bf16),
            pltpu.VMEM((n_tp, group, width), bf16),
            pltpu.VMEM((n_tp, blocks, head_dim), f32),
            pltpu.VMEM((n_tp, blocks, head_dim), f32),
            pltpu.VMEM((3, 2, kv_heads, head_dim), f32),
            pltpu.VMEM((n_tp, kv_heads, key_width), f32),
            pltpu.VMEM((count, group, width), bf16),
            pltpu.VMEM((n_ep * group, features), f32),
            pltpu.VMEM((count, group, width), bf16),
            pltpu.VMEM((count, group, width), bf16),
            pltpu.VMEM((group, width), bf16),
            pltpu.VMEM((kv_heads, key_width), bf16),
            pltpu.VMEM((kv_heads, key_width), bf16),
            dma((19,)),
            dma((3,)),
        ]
        + [dma((n_tp,))] * 6
        + [dma] * 4,
        compiler_params=pltpu.CompilerParams(
            collective_id=0, has_side_effects=True, vmem_limit_bytes=60 * 1024 * 1024
        ),
        name="fused_layer",
    )(*operands)
    return pl.pallas_call(
        hand_over,
        out_shape=tuple(jax.ShapeDtypeStruct(out.shape, out.dtype) for out in outs),
        in_specs=[pl.BlockSpec(memory_space=pltpu.VMEM)] * 3,
        out_specs=(pl.BlockSpec(memory_space=pltpu.VMEM),) * 3,
        name="hand_over",
    )(*outs)


def layer(n_ep, n_tp, *args):
    resid, cache_key, lambdas, w_gate = args[0], args[1], args[4], args[16]
    group, width = resid.shape
    sequences, kv_heads, _, key_width = cache_key.shape
    aligned = (
        sequences == 1
        and group == n_tp
        and n_tp > 1
        and lambdas.shape[0] == kv_heads
        and kv_heads % 8 == 0
        and key_width % 256 == 0
        and width % key_width == 0
        and w_gate.shape[0] == 1
        and n_ep * n_tp <= 32
    )
    if aligned:
        return fused_layer(n_ep, n_tp, *args)
    return local(*args)


def solution(mesh):
    in_specs = (
        P("ep", "tp"),
        P(("ep", "tp"), None, None, None),
        P(("ep", "tp"), None, None, None),
        P(("ep", "tp")),
        P(),
        P(),
        P(),
        P(),
        P(),
        P(),
        P(None, "tp"),
        P(None, "tp"),
        P(None, "tp"),
        P(None, "tp"),
        P("ep", None),
        P("ep", None),
        P("ep", None, "tp"),
        P("ep", None, "tp"),
        P("ep", "tp", None),
    )
    out_specs = (P("ep", "tp"), P(("ep", "tp"), None, None), P(("ep", "tp"), None, None))
    return jax.shard_map(functools.partial(layer, mesh.shape["ep"], mesh.shape["tp"]), mesh=mesh, in_specs=in_specs, out_specs=out_specs, check_vma=False)
```

```python
import functools
import math

import jax
import jax.numpy as jnp
from jax import lax
from jax.experimental import pallas as pl
from jax.experimental.pallas import tpu as pltpu
from jax.sharding import PartitionSpec as P

CAP = 4


epsilon = 1e-06
out_factor = 0.2 + 0.6 * math.exp(-0.3)
masked_score = -1e30


def scaled_rows(values, gain):
    wide = values.astype(jnp.float32)
    return wide * lax.rsqrt(jnp.mean(wide * wide, axis=-1, keepdims=True) + epsilon) * gain


def route_tables(routes, route_weights, experts, capacity):
    flat_routes = routes.reshape(-1)
    expert_hit = (flat_routes[:, None] == jnp.arange(experts, dtype=jnp.int32)[None, :]).astype(
        jnp.int32
    )
    before = jnp.cumsum(expert_hit, axis=0) - expert_hit
    slot_index = jnp.sum(before * expert_hit, axis=1)
    slot_hit = (slot_index[:, None] == jnp.arange(capacity, dtype=jnp.int32)[None, :]).astype(
        jnp.float32
    )
    pair_table = expert_hit.astype(jnp.float32)[:, :, None] * slot_hit[:, None, :]
    pair_table = pair_table.reshape(routes.shape[0], 2, experts, capacity)
    dispatch = jnp.sum(pair_table, axis=1)
    combine = jnp.sum(pair_table * route_weights[:, :, None, None], axis=1)
    return (dispatch, combine)


def attend(
    queries,
    key_rows,
    value_rows,
    past_keys,
    past_values,
    live_len,
    lambdas,
    query_gain,
    key_gain,
    sub_gain,
):
    seq_count, kv_heads, cache_len, key_width = past_keys.shape
    head_dim = key_width // 2
    head_count = lambdas.shape[0]
    group_size = head_count // kv_heads
    value_dim = past_values.shape[-1]
    score_scale = head_dim ** (-0.5)
    q_unit = scaled_rows(
        queries.reshape(seq_count, kv_heads, group_size, 2, head_dim), query_gain
    ).astype(jnp.bfloat16)
    new_key = scaled_rows(key_rows.reshape(seq_count, kv_heads, 2, head_dim), key_gain).astype(
        jnp.bfloat16
    )
    new_value = value_rows.reshape(seq_count, kv_heads, value_dim)
    past_split = past_keys.reshape(seq_count, kv_heads, cache_len, 2, head_dim)
    scores = (
        jnp.einsum("sjgmd,sjlmd->sjgml", q_unit, past_split, preferred_element_type=jnp.float32)
        * score_scale
    )
    own_score = (
        jnp.einsum("sjgmd,sjmd->sjgm", q_unit, new_key, preferred_element_type=jnp.float32)
        * score_scale
    )
    live_mask = jnp.arange(cache_len, dtype=jnp.int32)[None, :] < live_len[:, None]
    scores = jnp.where(live_mask[:, None, None, None, :], scores, masked_score)
    peak = jnp.maximum(jnp.max(scores, axis=-1), own_score)
    past_weight = jnp.exp(scores - peak[..., None])
    own_weight = jnp.exp(own_score - peak)
    totals = jnp.sum(past_weight, axis=-1) + own_weight
    past_prob = past_weight / totals[..., None]
    own_prob = own_weight / totals
    mix_lambda = lambdas.reshape(1, kv_heads, group_size, 1)
    past_mix = (past_prob[..., 0, :] - mix_lambda * past_prob[..., 1, :]).astype(jnp.bfloat16)
    own_mix = (own_prob[..., 0] - mix_lambda[..., 0] * own_prob[..., 1]).astype(jnp.bfloat16)
    head_out = jnp.einsum(
        "sjgl,sjlv->sjgv", past_mix, past_values, preferred_element_type=jnp.float32
    )
    head_out = (
        head_out
        + own_mix.astype(jnp.float32)[..., None] * new_value.astype(jnp.float32)[:, :, None, :]
    )
    mixed = (
        (scaled_rows(head_out, sub_gain) * out_factor)
        .astype(jnp.bfloat16)
        .reshape(seq_count, head_count * value_dim)
    )
    return (mixed, new_key.reshape(seq_count, kv_heads, key_width), new_value)


def local(
    resid,
    cache_key,
    cache_value,
    lengths,
    lambdas,
    mix_gain,
    query_gain,
    key_gain,
    sub_gain,
    ffn_gain,
    w_query,
    w_key,
    w_value,
    w_out,
    routes,
    route_weights,
    w_gate,
    w_up,
    w_down,
):
    gathered = lax.all_gather(resid, "tp", axis=1, tiled=True)
    normed = scaled_rows(gathered, mix_gain).astype(jnp.bfloat16)
    query_part = jnp.dot(normed, w_query, preferred_element_type=jnp.float32).astype(jnp.bfloat16)
    key_part = jnp.dot(normed, w_key, preferred_element_type=jnp.float32).astype(jnp.bfloat16)
    value_part = jnp.dot(normed, w_value, preferred_element_type=jnp.float32).astype(jnp.bfloat16)
    queries, key_rows, value_rows = (
        lax.all_to_all(query_part, "tp", split_axis=0, concat_axis=1, tiled=True),
        lax.all_to_all(key_part, "tp", split_axis=0, concat_axis=1, tiled=True),
        lax.all_to_all(value_part, "tp", split_axis=0, concat_axis=1, tiled=True),
    )
    mixed, new_key, new_value = attend(
        queries,
        key_rows,
        value_rows,
        cache_key,
        cache_value,
        lengths,
        lambdas,
        query_gain,
        key_gain,
        sub_gain,
    )
    attn_proj = jnp.dot(
        lax.all_gather(mixed, "tp", axis=0, tiled=True), w_out, preferred_element_type=jnp.float32
    )
    updated = (resid.astype(jnp.float32) + attn_proj).astype(jnp.bfloat16)
    updated_rows = lax.all_gather(updated, "tp", axis=1, tiled=True)
    hidden = scaled_rows(updated_rows, ffn_gain).astype(jnp.bfloat16)
    experts = w_gate.shape[0] * lax.axis_size("ep")
    dispatch, combine = route_tables(routes, route_weights, experts, CAP)
    send = jnp.einsum(
        "gec,gd->ecd", dispatch.astype(jnp.bfloat16), hidden, preferred_element_type=jnp.float32
    ).astype(jnp.bfloat16)
    slots = lax.all_to_all(send, "ep", split_axis=0, concat_axis=0, tiled=True)
    flat_rows = slots.reshape(-1, slots.shape[-1])
    gate_out = jnp.dot(flat_rows, w_gate[0], preferred_element_type=jnp.float32)
    up_out = jnp.dot(flat_rows, w_up[0], preferred_element_type=jnp.float32)
    act = (jax.nn.silu(gate_out) * up_out).astype(jnp.bfloat16)
    down_out = jnp.dot(act, w_down[0], preferred_element_type=jnp.float32)
    partial_value = down_out.reshape(slots.shape[0], slots.shape[1], down_out.shape[-1])
    flat_combine = combine.reshape(combine.shape[0], -1)
    summed = lax.psum_scatter(
        partial_value.astype(jnp.bfloat16), "tp", scatter_dimension=2, tiled=True
    ).astype(jnp.float32)
    returned = lax.all_to_all(
        summed.astype(jnp.bfloat16), "ep", split_axis=0, concat_axis=0, tiled=True
    ).astype(summed.dtype)
    expert_mix = jnp.dot(
        flat_combine,
        returned.reshape(-1, returned.shape[-1]),
        precision=lax.Precision.HIGHEST,
        preferred_element_type=jnp.float32,
    )
    result = (updated.astype(jnp.float32) + expert_mix).astype(jnp.bfloat16)
    return (result, new_key, new_value)


MESH = pl.DeviceIdType.MESH


def rms_scale(wide):
    return lax.rsqrt(jnp.mean(wide * wide, axis=-1, keepdims=True) + epsilon)


def fused(
    n_ep,
    n_tp,
    lengths,
    lambdas,
    resid,
    mix_gain,
    query_gain,
    key_gain,
    sub_gain,
    ffn_gain,
    routes,
    route_weights,
    w_query,
    w_key,
    w_value,
    cache_key,
    cache_value,
    w_out,
    w_gate,
    w_up,
    w_down,
    result,
    new_key,
    new_value,
    mix_gain_v,
    query_gain_v,
    key_gain_v,
    sub_gain_v,
    ffn_gain_v,
    lengths_v,
    lambdas_v,
    routes_v,
    weights_v,
    wq_v,
    wk_v,
    wv_v,
    ck_v,
    cv_v,
    wo_v,
    wg_v,
    wu_v,
    wd_v,
    res_all,
    proj_send,
    proj_all,
    heads_v,
    mix_all,
    upd_all,
    rows_v,
    part_send,
    part_all,
    result_v,
    new_key_v,
    new_value_v,
    load_sem,
    out_sem,
    res_s,
    res_r,
    proj_s,
    proj_r,
    mix_s,
    mix_r,
    upd_s,
    upd_r,
    part_s,
    part_r,
):
    f32, bf16 = jnp.float32, jnp.bfloat16
    ep, tp = lax.axis_index("ep"), lax.axis_index("tp")
    count = n_ep * n_tp
    me = ep * n_tp + tp
    group, width = resid.shape
    kv_heads, cache_len, key_width = ck_v.shape
    head_dim = key_width // 2
    heads_here = width // key_width

    loads = [
        (resid, res_all.at[tp]),
        (mix_gain, mix_gain_v),
        (w_query, wq_v),
        (w_key, wk_v),
        (w_value, wv_v),
        (query_gain, query_gain_v),
        (key_gain, key_gain_v),
        (sub_gain, sub_gain_v),
        (ffn_gain, ffn_gain_v),
        (lengths, lengths_v),
        (lambdas, lambdas_v),
        (routes, routes_v),
        (route_weights, weights_v),
        (cache_key.at[0], ck_v),
        (cache_value.at[0], cv_v),
        (w_out, wo_v),
        (w_gate.at[0], wg_v),
        (w_up.at[0], wu_v),
        (w_down.at[0], wd_v),
    ]
    copies = [
        pltpu.make_async_copy(source, target, load_sem.at[at])
        for at, (source, target) in enumerate(loads)
    ]
    for copy in copies[:5]:
        copy.start()
    (
        resid_c,
        mix_gain_c,
        wq_c,
        wk_c,
        wv_c,
        query_gain_c,
        key_gain_c,
        sub_gain_c,
        ffn_gain_c,
        lengths_c,
        lambdas_c,
        routes_c,
        weights_c,
        ck_c,
        cv_c,
        wo_c,
        wg_c,
        wu_c,
        wd_c,
    ) = copies

    barrier = pltpu.get_barrier_semaphore()

    for step in range(1, n_tp):
        pl.semaphore_signal(
            barrier, inc=1, device_id=(ep, lax.rem(tp + step, n_tp)), device_id_type=MESH
        )
    for step in range(1, n_ep):
        pl.semaphore_signal(
            barrier, inc=1, device_id=(lax.rem(ep + step, n_ep), tp), device_id_type=MESH
        )
    for copy in copies[5:]:
        copy.start()
    pl.semaphore_wait(barrier, n_tp + n_ep - 2)

    def tp_copy(step, source, target, send, recv):
        peer = lax.rem(tp + step, n_tp)
        return pltpu.make_async_remote_copy(
            src_ref=source(peer),
            dst_ref=target.at[tp],
            send_sem=send.at[step],
            recv_sem=recv.at[tp],
            device_id=(ep, peer),
            device_id_type=MESH,
        )

    def tp_wait(step, target, send, recv):
        peer = lax.rem(tp + step, n_tp)
        return pltpu.make_async_remote_copy(
            src_ref=target.at[peer],
            dst_ref=target.at[peer],
            send_sem=send.at[step],
            recv_sem=recv.at[peer],
            device_id=(ep, peer),
            device_id_type=MESH,
        )

    resid_c.wait()
    for step in range(1, n_tp):
        tp_copy(step, lambda peer: res_all.at[tp], res_all, res_s, res_r).start()
    mix_gain_c.wait()
    for step in range(1, n_tp):
        tp_wait(step, res_all, res_s, res_r).wait_recv()
    wide = jnp.concatenate([res_all[t].astype(f32) for t in range(n_tp)], axis=1)
    normed = (wide * rms_scale(wide) * mix_gain_v[...]).astype(bf16)

    blocks = 2 * heads_here
    for section, (copy, weight) in enumerate(((wq_c, wq_v), (wk_c, wk_v), (wv_c, wv_v))):
        copy.wait()
        out = jnp.dot(normed, weight[...], preferred_element_type=f32).astype(bf16).astype(f32)
        for head in range(heads_here):
            for half in range(2):
                at = (head * 2 + half) * head_dim
                proj_send[:, section * blocks + half * heads_here + head, :] = out[
                    :, at : at + head_dim
                ]
    for step in range(1, n_tp):
        tp_copy(step, lambda peer: proj_send.at[peer], proj_all, proj_s, proj_r).start()
    proj_all[tp] = proj_send[tp]
    for copy in (query_gain_c, key_gain_c, sub_gain_c, ffn_gain_c, lengths_c, lambdas_c, routes_c, weights_c):
        copy.wait()
    for step in range(1, n_tp):
        tp_wait(step, proj_all, proj_s, proj_r).wait_recv()
    for t in range(n_tp):
        for section in range(3):
            for half in range(2):
                at = section * blocks + half * heads_here
                heads_v[section, half, t * heads_here : (t + 1) * heads_here, :] = proj_all[
                    t, at : at + heads_here, :
                ]
    maps = 2 * kv_heads
    q_raw = heads_v[0].reshape(maps, head_dim)
    k_raw = heads_v[1].reshape(maps, head_dim)
    q_unit = (q_raw * rms_scale(q_raw) * query_gain_v[...]).astype(bf16).astype(f32)
    k_unit = (k_raw * rms_scale(k_raw) * key_gain_v[...]).astype(bf16).astype(f32)
    value_own = jnp.concatenate([heads_v[2, 0], heads_v[2, 1]], axis=1)
    new_key_v[...] = jnp.concatenate([k_unit[:kv_heads], k_unit[kv_heads:]], axis=1).astype(bf16)
    new_value_v[...] = value_own.astype(bf16)
    out_copies = [
        pltpu.make_async_copy(new_key_v, new_key.at[0], out_sem.at[0]),
        pltpu.make_async_copy(new_value_v, new_value.at[0], out_sem.at[1]),
    ]
    for copy in out_copies:
        copy.start()

    row = lax.broadcasted_iota(jnp.int32, (maps, 1), 0)
    head_row = lax.rem(row, kv_heads)
    first = row < kv_heads
    q_wide = jnp.concatenate(
        [jnp.where(first, q_unit, 0.0), jnp.where(first, 0.0, q_unit)], axis=1
    ).astype(bf16)
    ck_c.wait()
    scores = jnp.zeros((maps, cache_len), f32)
    for head in range(kv_heads):
        part = lax.dot_general(
            q_wide, ck_v[head], (((1,), (1,)), ((), ())), preferred_element_type=f32
        )
        scores = jnp.where(head_row == head, part, scores)
    scale = head_dim ** (-0.5)
    own_score = jnp.sum(q_unit * k_unit, axis=-1, keepdims=True) * scale
    live = lax.broadcasted_iota(jnp.int32, (maps, cache_len), 1) < lengths_v[0]
    scores = jnp.where(live, scores * scale, masked_score)
    peak = jnp.maximum(jnp.max(scores, axis=-1, keepdims=True), own_score)
    past_weight = jnp.exp(scores - peak)
    own_weight = jnp.exp(own_score - peak)
    totals = jnp.sum(past_weight, axis=-1, keepdims=True) + own_weight
    past_prob = past_weight / totals
    own_prob = own_weight / totals
    lam = jnp.zeros((kv_heads, 1), f32)
    for head in range(kv_heads):
        lam = jnp.where(row[:kv_heads] == head, lambdas_v[head], lam)
    past_mix = (past_prob[:kv_heads] - lam * past_prob[kv_heads:]).astype(bf16)
    own_mix = (own_prob[:kv_heads] - lam * own_prob[kv_heads:]).astype(bf16).astype(f32)
    cv_c.wait()
    head_out = jnp.zeros((kv_heads, key_width), f32)
    for head in range(kv_heads):
        part = jnp.dot(past_mix, cv_v[head], preferred_element_type=f32)
        head_out = jnp.where(row[:kv_heads] == head, part, head_out)
    head_out = head_out + own_mix * value_own
    mixed = (head_out * rms_scale(head_out) * sub_gain_v[...] * out_factor).astype(bf16)
    mix_all[tp] = mixed
    for step in range(1, n_tp):
        tp_copy(step, lambda peer: mix_all.at[tp], mix_all, mix_s, mix_r).start()
    wo_c.wait()
    for step in range(1, n_tp):
        tp_wait(step, mix_all, mix_s, mix_r).wait_recv()
    mixed_wide = mix_all[...].astype(f32)
    mixed_rows = jnp.concatenate([mixed_wide[:, head, :] for head in range(kv_heads)], axis=1)
    attn_proj = jnp.dot(mixed_rows.astype(bf16), wo_v[...], preferred_element_type=f32)
    updated = (res_all[tp].astype(f32) + attn_proj).astype(bf16)
    upd_all[me] = updated

    token = lax.broadcasted_iota(jnp.int32, (group, 128), 0)
    expert = lax.broadcasted_iota(jnp.int32, (group, 128), 1)
    shares = jnp.zeros((group, 128), f32)
    for s in range(group):
        for k in range(2):
            named = jnp.logical_and(token == s, expert == routes_v[k, s])
            shares = jnp.where(named, weights_v[k, s], shares)

    def any_copy(other, source, target, send, recv):
        return pltpu.make_async_remote_copy(
            src_ref=source,
            dst_ref=target.at[me],
            send_sem=send,
            recv_sem=recv,
            device_id=(other // n_tp, lax.rem(other, n_tp)),
            device_id_type=MESH,
        )

    def any_wait(target, send, recv):
        span = target.at[pl.ds(0, count - 1)]
        return pltpu.make_async_remote_copy(
            src_ref=span,
            dst_ref=span,
            send_sem=send,
            recv_sem=recv,
            device_id=(ep, tp),
            device_id_type=MESH,
        )

    def upd_start(step, carry):
        any_copy(lax.rem(me + count - step, count), upd_all.at[me], upd_all, upd_s, upd_r).start()
        return carry

    lax.fori_loop(1, count, upd_start, 0)

    wg_c.wait()
    wu_c.wait()
    wd_c.wait()
    any_wait(upd_all, upd_s, upd_r).wait_recv()
    for e in range(n_ep):
        for t in range(n_tp):
            rows_v[e * group : (e + 1) * group, t * width : (t + 1) * width] = upd_all[
                e * n_tp + t
            ].astype(f32)
    rows = rows_v[...]
    hidden = (rows * rms_scale(rows) * ffn_gain_v[...]).astype(bf16)
    gate_out = jnp.dot(hidden, wg_v[...], preferred_element_type=f32)
    up_out = jnp.dot(hidden, wu_v[...], preferred_element_type=f32)
    act = (jax.nn.silu(gate_out) * up_out).astype(bf16)

    for t in range(n_tp):
        slab = jnp.dot(act, wd_v[:, t * width : (t + 1) * width], preferred_element_type=f32)
        for e in range(n_ep):
            part_send[e * n_tp + t] = slab[e * group : (e + 1) * group].astype(bf16)

        def part_start(step, carry):
            other = lax.rem(ep + n_ep - 1 - step, n_ep) * n_tp + t

            @pl.when(other != me)
            def _():
                any_copy(other, part_send.at[other], part_all, part_s, part_r).start()

            return carry

        lax.fori_loop(0, n_ep, part_start, 0)
    part_all[me] = part_send[me]

    any_wait(part_all, part_s, part_r).wait_recv()
    expert_mix = jnp.zeros((group, width), f32)
    for e in range(n_ep):
        term = part_all[e * n_tp].astype(f32)
        for t in range(1, n_tp):
            term = term + part_all[e * n_tp + t].astype(f32)
        expert_mix = expert_mix + shares[:, e : e + 1] * term
    result_v[...] = (upd_all[me].astype(f32) + expert_mix).astype(bf16)
    out_copies.append(pltpu.make_async_copy(result_v, result, out_sem.at[2]))
    out_copies[2].start()

    for step in range(1, n_tp):
        tp_wait(step, res_all, res_s, res_r).wait_send()
        tp_wait(step, proj_all, proj_s, proj_r).wait_send()
        tp_wait(step, mix_all, mix_s, mix_r).wait_send()

    any_wait(upd_all, upd_s, upd_r).wait_send()
    any_wait(part_all, part_s, part_r).wait_send()
    for copy in out_copies:
        copy.wait()


def hand_over(*refs):
    for source, target in zip(refs[:3], refs[3:]):
        target[...] = source[...]


def fused_layer(n_ep, n_tp, *args):
    (
        resid,
        cache_key,
        cache_value,
        lengths,
        lambdas,
        mix_gain,
        query_gain,
        key_gain,
        sub_gain,
        ffn_gain,
        w_query,
        w_key,
        w_value,
        w_out,
        routes,
        route_weights,
        w_gate,
        w_up,
        w_down,
    ) = args
    bf16, f32 = jnp.bfloat16, jnp.float32
    group, width = resid.shape
    _, kv_heads, cache_len, key_width = cache_key.shape
    head_dim = key_width // 2
    features = width * n_tp
    hidden_units = w_gate.shape[2]
    count = n_ep * n_tp
    blocks = 6 * (width // key_width)
    any_spec = pl.BlockSpec(memory_space=pl.ANY)
    operands = (
        lengths,
        lambdas,
        resid,
        mix_gain.reshape(1, -1),
        query_gain.reshape(1, -1),
        key_gain.reshape(1, -1),
        sub_gain.reshape(1, -1),
        ffn_gain.reshape(1, -1),
        routes.T,
        route_weights.T,
        w_query,
        w_key,
        w_value,
        cache_key,
        cache_value,
        w_out,
        w_gate,
        w_up,
        w_down,
    )
    dma = pltpu.SemaphoreType.DMA
    outs = pl.pallas_call(
        functools.partial(fused, n_ep, n_tp),
        out_shape=(
            jax.ShapeDtypeStruct((group, width), bf16),
            jax.ShapeDtypeStruct((1, kv_heads, key_width), bf16),
            jax.ShapeDtypeStruct((1, kv_heads, key_width), bf16),
        ),
        in_specs=[any_spec] * len(operands),
        out_specs=(any_spec,) * 3,
        scratch_shapes=[
            pltpu.VMEM((1, features), f32),
            pltpu.VMEM((1, head_dim), f32),
            pltpu.VMEM((1, head_dim), f32),
            pltpu.VMEM((1, key_width), f32),
            pltpu.VMEM((1, features), f32),
            pltpu.SMEM(lengths.shape, jnp.int32),
            pltpu.SMEM(lambdas.shape, f32),
            pltpu.SMEM(routes.shape[::-1], jnp.int32),
            pltpu.SMEM(routes.shape[::-1], f32),
            pltpu.VMEM((features, width), bf16),
            pltpu.VMEM((features, width), bf16),
            pltpu.VMEM((features, width), bf16),
            pltpu.VMEM((kv_heads, cache_len, key_width), bf16),
            pltpu.VMEM((kv_heads, cache_len, key_width), bf16),
            pltpu.VMEM((features, width), bf16),
            pltpu.VMEM((features, hidden_units), bf16),
            pltpu.VMEM((features, hidden_units), bf16),
            pltpu.VMEM((hidden_units, features), bf16),
            pltpu.VMEM((n_tp, group, width), bf16),
            pltpu.VMEM((n_tp, blocks, head_dim), f32),
            pltpu.VMEM((n_tp, blocks, head_dim), f32),
            pltpu.VMEM((3, 2, kv_heads, head_dim), f32),
            pltpu.VMEM((n_tp, kv_heads, key_width), bf16),
            pltpu.VMEM((count, group, width), bf16),
            pltpu.VMEM((n_ep * group, features), f32),
            pltpu.VMEM((count, group, width), bf16),
            pltpu.VMEM((count, group, width), bf16),
            pltpu.VMEM((group, width), bf16),
            pltpu.VMEM((kv_heads, key_width), bf16),
            pltpu.VMEM((kv_heads, key_width), bf16),
            dma((19,)),
            dma((3,)),
        ]
        + [dma((n_tp,))] * 6
        + [dma] * 4,
        compiler_params=pltpu.CompilerParams(
            collective_id=0, has_side_effects=True, vmem_limit_bytes=60 * 1024 * 1024
        ),
        name="fused_layer",
    )(*operands)
    return pl.pallas_call(
        hand_over,
        out_shape=tuple(jax.ShapeDtypeStruct(out.shape, out.dtype) for out in outs),
        in_specs=[pl.BlockSpec(memory_space=pltpu.VMEM)] * 3,
        out_specs=(pl.BlockSpec(memory_space=pltpu.VMEM),) * 3,
        name="hand_over",
    )(*outs)


def layer(n_ep, n_tp, *args):
    resid, cache_key, lambdas, w_gate = args[0], args[1], args[4], args[16]
    group, width = resid.shape
    sequences, kv_heads, _, key_width = cache_key.shape
    aligned = (
        sequences == 1
        and group == n_tp
        and n_tp > 1
        and lambdas.shape[0] == kv_heads
        and kv_heads % 8 == 0
        and key_width % 256 == 0
        and width % key_width == 0
        and w_gate.shape[0] == 1
        and n_ep * n_tp <= 32
    )
    if aligned:
        return fused_layer(n_ep, n_tp, *args)
    return local(*args)


def solution(mesh):
    in_specs = (
        P("ep", "tp"),
        P(("ep", "tp"), None, None, None),
        P(("ep", "tp"), None, None, None),
        P(("ep", "tp")),
        P(),
        P(),
        P(),
        P(),
        P(),
        P(),
        P(None, "tp"),
        P(None, "tp"),
        P(None, "tp"),
        P(None, "tp"),
        P("ep", None),
        P("ep", None),
        P("ep", None, "tp"),
        P("ep", None, "tp"),
        P("ep", "tp", None),
    )
    out_specs = (P("ep", "tp"), P(("ep", "tp"), None, None), P(("ep", "tp"), None, None))
    return jax.shard_map(functools.partial(layer, mesh.shape["ep"], mesh.shape["tp"]), mesh=mesh, in_specs=in_specs, out_specs=out_specs, check_vma=False)
```
